32 devices in a mesh: sp: 8 (over z, y), tp: 4 (over x, core).
Axes of the slice: x: 2, y: 2, z: 4, core: 2. Of those that a mesh axis runs over, the one named last changes fastest.
Arguments:
- residual: bfloat16 [2048, 2048], P('sp'), may hold values from -6 to 6
- ssm_input: bfloat16 [2048, 1024], P('sp', 'tp'), may hold values from -6 to 6
- in_map: bfloat16 [2, 64, 16, 128], P(None, 'tp'), may hold values from -1 to 1
- out_map: bfloat16 [2, 64, 16, 128], P(None, 'tp'), may hold values from -0.5 to 0.5
- damping: float32 [64, 64], P('tp'), may hold values from 0.0001 to 0.24
- log_step: float32 [64], P('tp'), may hold values from -8 to -1.2
- frequency: float32 [64, 64], P('tp'), may hold values from 1 to 201.06177
- pacing: float32 [2048], P('sp'), may hold values from 0.28 to 3.5
- feedthrough: float32 [1024], P('tp'), may hold values from -4 to 4
- w_out: bfloat16 [1024, 2048], P('tp'), may hold values from -0.375 to 0.375
- gain_mix: float32 [2048], replicated, may hold values from 0.1 to 1.9
- w_gate: bfloat16 [2048, 5632], P('sp', 'tp'), may hold values from -0.125 to 0.125
- w_value: bfloat16 [2048, 5632], P('sp', 'tp'), may hold values from -0.125 to 0.125
- conv_taps: float32 [3, 5632], P(None, 'tp'), may hold values from -3 to 3
- w_down: bfloat16 [5632, 2048], P('tp', 'sp'), may hold values from -0.21875 to 0.21875
- gain_ffn: float32 [2048], replicated, may hold values from 0.1 to 1.9
Outputs:
- result: bfloat16 [2048, 2048], P(('sp', 'tp'))
The draws below stay inside these ranges and needn't reach their ends.
All inputs are finite; a program needn't handle non-finite values.
Results may differ from the reference program's by a relative error of at most 0.02.
Values may be sent and summed in bfloat16 or wider, within the bound.
No kernel may reach another device: no remote copies, remote signals or barrier semaphores. Data moves between devices by JAX's collectives and lax.ppermute only.
A program may use at most 128 MiB of HBM per device.

```python
import math
import jax
import jax.numpy as jnp
from jax import lax

MODEL = 2048
CHANNELS = 1024
GROUP_CH = 16
STATES = 64
FF_UNITS = 5632
GROUPS = 64
LENGTH = 2048
N_TP = 4


def group_law(key):
    keys = jax.random.split(jax.random.fold_in(key, 11), 4)
    fast_share = 0.5
    fast = jax.random.uniform(keys[0], (GROUPS,), jnp.float32) < fast_share
    fast_step = jnp.exp(jax.random.uniform(keys[1], (GROUPS,), jnp.float32, jnp.log(0.2), jnp.log(0.3)))
    slow_rate = jnp.exp(jax.random.uniform(keys[2], (GROUPS,), jnp.float32, jnp.log(0.2), 0.0)) / LENGTH
    slow_step = jnp.sqrt(slow_rate / 0.6)
    step_size = jnp.where(fast, fast_step, slow_step)
    ratio = jax.random.uniform(keys[3], (GROUPS, STATES), jnp.float32, 0.4, 0.8)
    return (step_size, ratio)


def draw_log_step(key, part):
    step_size, ratio = group_law(key)
    return jnp.log(step_size)


def draw_damping(key, part):
    step_size, ratio = group_law(key)
    return step_size[:, None] * ratio


def draw_pacing(key, part):
    keys = jax.random.split(jax.random.fold_in(key, 23), 2)
    spans = LENGTH // 256 + 1
    coarse = jnp.exp(jax.random.uniform(keys[0], (spans,), jnp.float32, jnp.log(0.4), jnp.log(2.5)))
    finer = jnp.exp(jax.random.uniform(keys[1], (LENGTH,), jnp.float32, jnp.log(0.7), jnp.log(1.4)))
    return coarse[jnp.arange(LENGTH) // 256] * finer


def levels(stream_key, shape, pieces, least, high):
    gain = 1.0
    for position, blocks in pieces:
        steps = jax.random.uniform(jax.random.fold_in(jax.random.fold_in(stream_key, 6), position), (blocks,), jnp.float32, least / len(pieces), high / len(pieces))
        gain = gain * jnp.repeat(jnp.exp(steps), shape[position] // blocks).reshape((-1,) + (1,) * (len(shape) - 1 - position))
    return gain


def normal_values(key, dims, scale, most, shards=(), held_as=jnp.bfloat16):
    gain = levels(key, dims, shards, -0.22, 0.18) if shards else 1.0
    drawn = jax.random.normal(key, dims, jnp.float32) * scale * gain
    return jnp.minimum(jnp.maximum(drawn, -most), most).astype(held_as)


def setup_inputs(seed: int = 0) -> dict:
    seeds = jax.random.split(jax.random.key(seed), 17)
    return {
        "residual": normal_values(seeds[0], (LENGTH, MODEL), 1.0, 6.0, ((0, 8),)),
        "ssm_input": normal_values(seeds[1], (LENGTH, CHANNELS), 1.0, 6.0, ((0, 8), (1, 4))),
        "in_map": normal_values(seeds[2], (2, GROUPS, GROUP_CH, 2 * STATES), (2 * GROUP_CH) ** -0.5, 1.0, ((1, 4),)),
        "out_map": normal_values(seeds[3], (2, GROUPS, GROUP_CH, 2 * STATES), (2 * STATES) ** -0.5, 0.5, ((1, 4),)),
        "damping": draw_damping(jax.random.fold_in(seeds[16], 71), 0),
        "log_step": draw_log_step(jax.random.fold_in(seeds[16], 71), 0),
        "frequency": jnp.clip(1.0 + 200.06177 * jax.random.uniform(seeds[6], (GROUPS, STATES), jnp.float32) ** levels(seeds[6], (GROUPS, STATES), ((0, 4),), -0.2, 0.2), 1.0, 201.06177),
        "pacing": draw_pacing(jax.random.fold_in(seeds[16], 71), 0),
        "feedthrough": normal_values(seeds[8], (CHANNELS,), 1.0, 4.0, ((0, 4),), jnp.float32),
        "w_out": normal_values(seeds[9], (CHANNELS, MODEL), (CHANNELS // 4) ** -0.5, 0.375, ((0, 4),)),
        "gain_mix": jnp.clip(1.0 + 0.18 * jax.random.normal(seeds[10], (MODEL,), jnp.float32), 0.1, 1.9),
        "w_gate": normal_values(seeds[11], (MODEL, FF_UNITS), MODEL ** -0.5, 0.125, ((0, 8), (1, 4))),
        "w_value": normal_values(seeds[12], (MODEL, FF_UNITS), MODEL ** -0.5, 0.125, ((0, 8), (1, 4))),
        "conv_taps": normal_values(seeds[13], (3, FF_UNITS), 0.577, 3.0, ((1, 4),), jnp.float32),
        "w_down": normal_values(seeds[14], (FF_UNITS, MODEL), (FF_UNITS // 8) ** -0.5, 0.21875, ((0, 4), (1, 8))),
        "gain_ffn": jnp.clip(1.0 + 0.18 * jax.random.normal(seeds[15], (MODEL,), jnp.float32), 0.1, 1.9),
    }


deep_alpha = 8.0 ** 0.25
norm_eps = 1e-06
highest = lax.Precision.HIGHEST

def normalize(pre_norm, gain_row):
    mean_row = lax.optimization_barrier(jnp.mean(pre_norm, axis=-1, keepdims=True))
    centred = pre_norm - mean_row
    spread = lax.optimization_barrier(jnp.mean(centred * centred, axis=-1, keepdims=True))
    return centred * lax.rsqrt(spread + norm_eps) * gain_row

def complex_mul(a_re, a_im, b_re, b_im):
    return (a_re * b_re - a_im * b_im, a_re * b_im + a_im * b_re)

def one_direction(u_groups, pacing, in_map_d, out_map_d, damping, frequency, step_size, backward):
    length = u_groups.shape[0]
    groups = u_groups.shape[1]
    group_width = u_groups.shape[2]
    state_half = damping.shape[1]
    block_len = math.gcd(length, 512)
    blocks = length // block_len
    rate_re = -damping
    rate_im = frequency
    modulus = rate_re * rate_re + rate_im * rate_im
    in_full = in_map_d.astype(jnp.float32)
    out_full = out_map_d.astype(jnp.float32)

    def per_block(state_pair, inputs_now):
        u_block, pace_block = inputs_now
        inflow = jnp.einsum('tgc,gcq->tgq', u_block, in_full, precision=highest)
        deltas = step_size[None, :, None] * pace_block[:, None, None]
        magnitude = jnp.exp(rate_re[None] * deltas)
        decay_re = magnitude * jnp.cos(rate_im[None] * deltas)
        decay_im = magnitude * jnp.sin(rate_im[None] * deltas)
        less_one = decay_re - 1.0
        factor_re = (less_one * rate_re + decay_im * rate_im) / modulus
        factor_im = (decay_im * rate_re - less_one * rate_im) / modulus
        drive_re, drive_im = complex_mul(factor_re, factor_im, inflow[..., :state_half], inflow[..., state_half:])

        def advance(carry_pair, step_terms):
            old_re, old_im = carry_pair
            dec_re, dec_im, add_re, add_im = step_terms
            new_re, new_im = complex_mul(dec_re, dec_im, old_re, old_im)
            new_re = new_re + add_re
            new_im = new_im + add_im
            return ((new_re, new_im), jnp.concatenate([new_re, new_im], axis=-1))
        state_pair, sequence = lax.scan(advance, state_pair, (decay_re, decay_im, drive_re, drive_im), reverse=backward)
        readout = jnp.einsum('tgq,gcq->tgc', sequence, out_full, precision=highest)
        return (state_pair, readout)
    empty_state = jnp.zeros((groups, state_half), jnp.float32)
    u_blocks = u_groups.reshape(blocks, block_len, groups, group_width)
    pace_blocks = pacing.reshape(blocks, block_len)
    final_pair, readouts = lax.scan(per_block, (empty_state, empty_state), (u_blocks, pace_blocks), reverse=backward)
    return readouts.reshape(length, groups, group_width)

def blockwise(rows_in, weights):
    block_width = rows_in.shape[1] // N_TP
    running = jnp.zeros((rows_in.shape[0], weights.shape[1]), jnp.float32)
    for block_index in range(N_TP):
        first_col = block_index * block_width
        partial_value = jnp.dot(rows_in[:, first_col:first_col + block_width], weights[first_col:first_col + block_width], preferred_element_type=jnp.float32)
        running = running + lax.optimization_barrier(partial_value.astype(jnp.bfloat16)).astype(jnp.float32)
    return running

def reference(residual, ssm_input, in_map, out_map, damping, log_step, frequency, pacing, feedthrough, w_out, gain_mix, w_gate, w_value, conv_taps, w_down, gain_ffn):
    length = ssm_input.shape[0]
    channel_count = ssm_input.shape[1]
    groups = damping.shape[0]
    group_width = channel_count // groups
    step_size = jnp.exp(log_step)
    inputs_f = ssm_input.astype(jnp.float32)
    u_groups = inputs_f.reshape(length, groups, group_width)
    readout = one_direction(u_groups, pacing, in_map[0], out_map[0], damping, frequency, step_size, False)
    readout = readout + one_direction(u_groups, pacing, in_map[1], out_map[1], damping, frequency, step_size, True)
    readout = readout.reshape(length, channel_count) + feedthrough * inputs_f
    channels = jax.nn.gelu(readout).astype(jnp.bfloat16)
    mixed = blockwise(channels, w_out)
    norm_first = normalize(deep_alpha * residual.astype(jnp.float32) + mixed, gain_mix)
    norm_first = lax.optimization_barrier(norm_first.astype(jnp.bfloat16))
    ff_block = w_gate.shape[1] // N_TP
    branch = jnp.zeros(residual.shape, jnp.float32)
    for block_index in range(N_TP):
        first_col = block_index * ff_block
        gated = jnp.dot(norm_first, w_gate[:, first_col:first_col + ff_block], preferred_element_type=jnp.float32)
        gated = lax.optimization_barrier(gated.astype(jnp.bfloat16))
        values = jnp.dot(norm_first, w_value[:, first_col:first_col + ff_block], preferred_element_type=jnp.float32)
        values = lax.optimization_barrier(values.astype(jnp.bfloat16))
        padded = jnp.pad(gated.astype(jnp.float32), ((1, 1), (0, 0)))
        taps_now = conv_taps[:, first_col:first_col + ff_block]
        smoothed = taps_now[0] * padded[:-2] + taps_now[1] * padded[1:-1] + taps_now[2] * padded[2:]
        hidden = (jax.nn.gelu(smoothed) * values.astype(jnp.float32)).astype(jnp.bfloat16)
        partial_value = jnp.dot(hidden, w_down[first_col:first_col + ff_block], preferred_element_type=jnp.float32)
        branch = branch + lax.optimization_barrier(partial_value.astype(jnp.bfloat16)).astype(jnp.float32)
    result = normalize(deep_alpha * norm_first.astype(jnp.float32) + branch, gain_ffn)
    return result.astype(jnp.bfloat16)
```

```python
import math

import jax
import jax.numpy as jnp
from jax import lax
from jax.experimental import pallas as pl
from jax.experimental.pallas import tpu as pltpu
from jax.sharding import PartitionSpec as P

deep_alpha = 8.0**0.25
norm_eps = 1e-06
SEG = 8
LANES = 128
f32 = jnp.float32
bf16 = jnp.bfloat16
NT = (((1,), (1,)), ((), ()))


def vmem(limit=56):
    return pltpu.CompilerParams(vmem_limit_bytes=limit * 1024 * 1024)


def cost(flops, moved):
    return pl.CostEstimate(flops=flops, bytes_accessed=moved, transcendentals=0)


def whole_spec():
    return pl.BlockSpec(memory_space=pltpu.VMEM)


def scalar_spec():
    return pl.BlockSpec(memory_space=pltpu.SMEM)


def iota(shape, dim):
    return lax.broadcasted_iota(jnp.int32, shape, dim)


def cmul(a_re, a_im, b_re, b_im):
    return a_re * b_re - a_im * b_im, a_re * b_im + a_im * b_re


def sin_cos(angle):
    turns = jnp.floor(angle * (2.0 / math.pi) + 0.5)
    rest = ((angle - turns * 1.5703125) - turns * 4.837512969970703125e-4) - (
        turns * 7.54978995489188216e-8
    )
    sq = rest * rest
    sine = ((-1.9515295891e-4 * sq + 8.3321608736e-3) * sq - 1.6666654611e-1) * sq * rest + rest
    cosine = (
        ((2.443315711809948e-5 * sq - 1.388731625493765e-3) * sq + 4.166664568298827e-2) * sq * sq
        - 0.5 * sq
        + 1.0
    )
    quad = turns.astype(jnp.int32)
    swap = (quad & 1) == 1
    sin_out = jnp.where(swap, cosine, sine)
    cos_out = jnp.where(swap, sine, cosine)
    sin_out = jnp.where((quad & 2) == 2, -sin_out, sin_out)
    cos_out = jnp.where(((quad + 1) & 2) == 2, -cos_out, cos_out)
    return sin_out, cos_out


def spread_maps(maps, group_width):
    half = LANES // 2
    rows = maps[0].shape[0]
    lane = iota((rows, LANES), 1)
    low = lane < half
    odd = (iota((rows, LANES), 0) // group_width) % 2 == 1
    match = odd != low
    parts = []
    for one in maps:
        one = one.astype(f32)
        turned = pltpu.roll(one, half, 1)
        parts.append(jnp.where(match, jnp.where(low, one, turned), 0.0))
        parts.append(jnp.where(match, jnp.where(low, turned, one), 0.0))
    return jnp.concatenate(parts, axis=1).astype(bf16)


def state_kernel(
    u_ref, in_ref, out_ref, damp_ref, freq_ref, logs_ref, pace_ref,
    ro_ref, dec_ref, seg_ref, sum_ref,
    tab, wide_in, wide_out, u_perm, drv, st, pc,
):
    length = u_ref.shape[0]
    groups = damp_ref.shape[0]
    half = damp_ref.shape[1]
    width = u_ref.shape[1] // groups
    steps = length // SEG
    tiles = groups // 2
    step = jnp.exp(logs_ref[...])
    diag = iota((groups, groups), 0) == iota((groups, groups), 1)
    step_col = jnp.sum(jnp.where(diag, jnp.broadcast_to(step, (groups, groups)), 0.0), axis=1, keepdims=True)
    rate_re = -damp_ref[...]
    rate_im = freq_ref[...]
    modulus = rate_re * rate_re + rate_im * rate_im
    rows = (rate_re * step_col, rate_im * step_col, rate_re / modulus, -rate_im / modulus)
    low = iota((1, LANES), 1) < half
    for which, table in enumerate(rows):
        twice = jnp.concatenate([table, table], axis=1)
        for k in range(tiles):
            tab[k, which : which + 1, :] = jnp.where(low, twice[2 * k : 2 * k + 1], twice[2 * k + 1 : 2 * k + 2])
    wide_in[...] = spread_maps((in_ref[0], in_ref[1]), width)
    wide_out[...] = spread_maps((out_ref[0], out_ref[1]), width)
    r_id = iota((length, length), 0)
    t_id = iota((length, length), 1)
    pick = t_id == (r_id % SEG) * steps + r_id // SEG
    u_perm[...] = jnp.dot(
        jnp.where(pick, 1.0, 0.0).astype(bf16), u_ref[...], preferred_element_type=f32
    ).astype(bf16)
    pace_col = jnp.sum(
        jnp.where(pick, jnp.broadcast_to(pace_ref[...], (length, length)), 0.0), axis=1, keepdims=True
    )
    pc[...] = jnp.broadcast_to(pace_col, (length, LANES))
    ro_ref[...] = jnp.zeros_like(ro_ref)
    col_tile = iota((length, u_ref.shape[1]), 1) // (2 * width)

    def per_tile(k, carry):
        pace = pc[...]
        magnitude = jnp.exp(tab[k, 0:1, :] * pace)
        sine, cosine = sin_cos(tab[k, 1:2, :] * pace)
        dec_re = magnitude * cosine
        dec_im = magnitude * sine
        dec_ref[0, k] = dec_re
        dec_ref[1, k] = dec_im
        inv_re = tab[k, 2:3, :]
        inv_im = tab[k, 3:4, :]
        fac_re, fac_im = cmul(dec_re - 1.0, dec_im, inv_re, inv_im)
        mine = jnp.where(col_tile == k, u_perm[...].astype(f32), 0.0).astype(bf16)
        inflow = jnp.dot(mine, wide_in[...], preferred_element_type=f32)
        for d in range(2):
            x_re = inflow[:, 2 * d * LANES : (2 * d + 1) * LANES]
            x_im = inflow[:, (2 * d + 1) * LANES : (2 * d + 2) * LANES]
            a, b = cmul(fac_re, fac_im, x_re, x_im)
            drv[2 * d] = a
            drv[2 * d + 1] = b
        h_re = jnp.zeros((SEG, LANES), f32)
        h_im = h_re
        g_re = h_re
        g_im = h_re
        p_re = jnp.ones((SEG, LANES), f32)
        p_im = h_re
        for i in range(steps):
            lo = i * SEG
            d_re = dec_ref[0, k, lo : lo + SEG, :]
            d_im = dec_ref[1, k, lo : lo + SEG, :]
            h_re, h_im = cmul(d_re, d_im, h_re, h_im)
            h_re = h_re + drv[0, lo : lo + SEG, :]
            h_im = h_im + drv[1, lo : lo + SEG, :]
            st[lo : lo + SEG, 0:LANES] = h_re
            st[lo : lo + SEG, LANES : 2 * LANES] = h_im
            p_re, p_im = cmul(d_re, d_im, p_re, p_im)
            hi = (steps - 1 - i) * SEG
            d_re = dec_ref[0, k, hi : hi + SEG, :]
            d_im = dec_ref[1, k, hi : hi + SEG, :]
            g_re, g_im = cmul(d_re, d_im, g_re, g_im)
            g_re = g_re + drv[2, hi : hi + SEG, :]
            g_im = g_im + drv[3, hi : hi + SEG, :]
            st[hi : hi + SEG, 2 * LANES : 3 * LANES] = g_re
            st[hi : hi + SEG, 3 * LANES : 4 * LANES] = g_im
        ends = (p_re, p_im, h_re, h_im, g_re, g_im)
        for q in range(6):
            seg_ref[k, q] = ends[q]
        t_re = jnp.ones((1, LANES), f32)
        t_im = jnp.zeros((1, LANES), f32)
        f_re = t_im
        f_im = t_im
        b_re = t_im
        b_im = t_im
        for j in range(SEG):
            one = [e[j : j + 1] for e in ends]
            t_re, t_im = cmul(one[0], one[1], t_re, t_im)
            f_re, f_im = cmul(one[0], one[1], f_re, f_im)
            f_re = f_re + one[2]
            f_im = f_im + one[3]
            o = SEG - 1 - j
            one = [e[o : o + 1] for e in ends]
            b_re, b_im = cmul(one[0], one[1], b_re, b_im)
            b_re = b_re + one[4]
            b_im = b_im + one[5]
        for q, row in enumerate((t_re, t_im, f_re, f_im, b_re, b_im)):
            sum_ref[q, pl.ds(k, 1), :] = row
        states = st[...]
        upper = states.astype(bf16)
        lower = (states - upper.astype(f32)).astype(bf16)
        got = lax.dot_general(upper, wide_out[...], NT, preferred_element_type=f32)
        got = got + lax.dot_general(lower, wide_out[...], NT, preferred_element_type=f32)
        ro_ref[...] = jnp.where(col_tile == k, got, ro_ref[...])
        return carry

    lax.fori_loop(0, tiles, per_tile, 0)


def carry_kernel(
    ids_ref, dec_ref, seg_ref, gat_ref, ro_ref, u_ref, feed_ref, out_ref,
    ch_ref,
    wide_out, acc, st, car, pad, *, count, relative,
):
    length = u_ref.shape[0]
    channels = u_ref.shape[1]
    tiles = dec_ref.shape[1]
    width = channels // (2 * tiles)
    steps = length // SEG
    mine = ids_ref[0]
    wide_out[...] = spread_maps((out_ref[0], out_ref[1]), width)
    zero = jnp.zeros((tiles, LANES), f32)

    def fold(n, state):
        f_re, f_im, b_re, b_im = state
        here = n
        at = jnp.bitwise_xor(here, mine) if relative else here
        a, b = cmul(gat_ref[at, 0], gat_ref[at, 1], f_re, f_im)
        ok = here < mine
        f_re = jnp.where(ok, a + gat_ref[at, 2], f_re)
        f_im = jnp.where(ok, b + gat_ref[at, 3], f_im)
        here = count - 1 - n
        at = jnp.bitwise_xor(here, mine) if relative else here
        a, b = cmul(gat_ref[at, 0], gat_ref[at, 1], b_re, b_im)
        ok = here > mine
        b_re = jnp.where(ok, a + gat_ref[at, 4], b_re)
        b_im = jnp.where(ok, b + gat_ref[at, 5], b_im)
        return f_re, f_im, b_re, b_im

    for q, value in enumerate(lax.fori_loop(0, count, fold, (zero, zero, zero, zero))):
        car[q] = value
    acc[...] = ro_ref[...]
    col_tile = iota((length, channels), 1) // (2 * width)

    def per_tile(k, carry):
        f_re = car[0, pl.ds(k, 1), :]
        f_im = car[1, pl.ds(k, 1), :]
        b_re = car[2, pl.ds(k, 1), :]
        b_im = car[3, pl.ds(k, 1), :]
        for j in range(SEG):
            pad[0, j : j + 1, :] = f_re
            pad[1, j : j + 1, :] = f_im
            a, b = cmul(seg_ref[k, 0, j : j + 1, :], seg_ref[k, 1, j : j + 1, :], f_re, f_im)
            f_re = a + seg_ref[k, 2, j : j + 1, :]
            f_im = b + seg_ref[k, 3, j : j + 1, :]
            o = SEG - 1 - j
            pad[2, o : o + 1, :] = b_re
            pad[3, o : o + 1, :] = b_im
            a, b = cmul(seg_ref[k, 0, o : o + 1, :], seg_ref[k, 1, o : o + 1, :], b_re, b_im)
            b_re = a + seg_ref[k, 4, o : o + 1, :]
            b_im = b + seg_ref[k, 5, o : o + 1, :]
        h_re = pad[0]
        h_im = pad[1]
        g_re = pad[2]
        g_im = pad[3]
        for i in range(steps):
            lo = i * SEG
            h_re, h_im = cmul(dec_ref[0, k, lo : lo + SEG, :], dec_ref[1, k, lo : lo + SEG, :], h_re, h_im)
            st[lo : lo + SEG, 0:LANES] = h_re
            st[lo : lo + SEG, LANES : 2 * LANES] = h_im
            hi = (steps - 1 - i) * SEG
            g_re, g_im = cmul(dec_ref[0, k, hi : hi + SEG, :], dec_ref[1, k, hi : hi + SEG, :], g_re, g_im)
            st[hi : hi + SEG, 2 * LANES : 3 * LANES] = g_re
            st[hi : hi + SEG, 3 * LANES : 4 * LANES] = g_im
        states = st[...]
        upper = states.astype(bf16)
        lower = (states - upper.astype(f32)).astype(bf16)
        got = lax.dot_general(upper, wide_out[...], NT, preferred_element_type=f32)
        got = got + lax.dot_general(lower, wide_out[...], NT, preferred_element_type=f32)
        acc[...] = acc[...] + jnp.where(col_tile == k, got, 0.0)
        return carry

    lax.fori_loop(0, tiles, per_tile, 0)
    r_id = iota((length, length), 0)
    t_id = iota((length, length), 1)
    pick = jnp.where(t_id == (r_id % SEG) * steps + r_id // SEG, 1.0, 0.0).astype(bf16)
    u_perm = jnp.dot(pick, u_ref[...], preferred_element_type=f32)
    made = jax.nn.gelu(acc[...] + feed_ref[...] * u_perm).astype(bf16)
    unpick = jnp.where(r_id == (t_id % SEG) * steps + t_id // SEG, 1.0, 0.0).astype(bf16)
    ch_ref[...] = jnp.dot(unpick, made, preferred_element_type=f32).astype(bf16)


def ssm_channels(ssm_input, in_map, out_map, damping, log_step, frequency, pacing, feedthrough):
    length, channels = ssm_input.shape
    groups, half = damping.shape
    tiles = groups // 2
    count = lax.axis_size("sp")
    in_rows = in_map.reshape(2, channels, 2 * half)
    out_rows = out_map.reshape(2, channels, 2 * half)
    ro, dec, seg, summary = pl.pallas_call(
        state_kernel,
        out_shape=(
            jax.ShapeDtypeStruct((length, channels), f32),
            jax.ShapeDtypeStruct((2, tiles, length, LANES), f32),
            jax.ShapeDtypeStruct((tiles, 6, SEG, LANES), f32),
            jax.ShapeDtypeStruct((6, tiles, LANES), f32),
        ),
        in_specs=[whole_spec()] * 7,
        out_specs=[whole_spec()] * 4,
        scratch_shapes=[
            pltpu.VMEM((tiles, 8, LANES), f32),
            pltpu.VMEM((channels, 4 * LANES), bf16),
            pltpu.VMEM((channels, 4 * LANES), bf16),
            pltpu.VMEM((length, channels), bf16),
            pltpu.VMEM((4, length, LANES), f32),
            pltpu.VMEM((length, 4 * LANES), f32),
            pltpu.VMEM((length, LANES), f32),
        ],
        compiler_params=vmem(),
        cost_estimate=cost(2_000_000_000, 4_000_000),
        name="state_pass",
    )(
        ssm_input, in_rows, out_rows, damping, frequency,
        log_step.reshape(1, groups), pacing.reshape(1, length),
    )
    relative = count & (count - 1) == 0 and count <= 16
    if relative:
        gathered = summary[None]
        step = 1
        while step < count:
            other = lax.ppermute(gathered, "sp", [(i, i ^ step) for i in range(count)])
            gathered = jnp.concatenate([gathered, other], axis=0)
            step *= 2
    else:
        gathered = lax.all_gather(summary, "sp")
    ids = jnp.stack([lax.axis_index("sp")]).astype(jnp.int32)

    def body(*refs):
        carry_kernel(*refs, count=count, relative=relative)

    return pl.pallas_call(
        body,
        out_shape=jax.ShapeDtypeStruct((length, channels), bf16),
        in_specs=[scalar_spec()] + [whole_spec()] * 7,
        out_specs=whole_spec(),
        scratch_shapes=[
            pltpu.VMEM((channels, 4 * LANES), bf16),
            pltpu.VMEM((length, channels), f32),
            pltpu.VMEM((length, 4 * LANES), f32),
            pltpu.VMEM((4, tiles, LANES), f32),
            pltpu.VMEM((4, SEG, LANES), f32),
        ],
        compiler_params=vmem(),
        cost_estimate=cost(2_000_000_000, 4_000_000),
        name="carry_pass",
    )(ids, dec, seg, gathered, ro, ssm_input, feedthrough.reshape(1, channels), out_rows)


def normalize(pre_norm, gain_row):
    mean_row = jnp.mean(pre_norm, axis=-1, keepdims=True)
    centred = pre_norm - mean_row
    spread = jnp.mean(centred * centred, axis=-1, keepdims=True)
    return centred * lax.rsqrt(spread + norm_eps) * gain_row


def plain_mixer(channels, residual, w_out, gain_mix, w_gate, w_value, conv_taps, w_down, gain_ffn):
    own_rows = residual.shape[0] // lax.axis_size("tp")
    mixed = lax.psum(
        jnp.dot(channels, w_out, preferred_element_type=f32).astype(bf16), "tp"
    ).astype(f32)
    rows = normalize(deep_alpha * residual.astype(f32) + mixed, gain_mix).astype(bf16)
    kept = lax.dynamic_slice_in_dim(rows, lax.axis_index("tp") * own_rows, own_rows, 0).astype(f32)
    gated = jnp.dot(
        rows, lax.all_gather(w_gate, "sp", axis=0, tiled=True), preferred_element_type=f32
    ).astype(bf16)
    values = jnp.dot(
        rows, lax.all_gather(w_value, "sp", axis=0, tiled=True), preferred_element_type=f32
    ).astype(bf16)
    count = lax.axis_size("sp")
    before = lax.ppermute(gated[-1:], "sp", [(i, i + 1) for i in range(count - 1)])
    after = lax.ppermute(gated[:1], "sp", [(i + 1, i) for i in range(count - 1)])
    padded = jnp.concatenate([before, gated, after], axis=0).astype(f32)
    smoothed = conv_taps[0] * padded[:-2] + conv_taps[1] * padded[1:-1] + conv_taps[2] * padded[2:]
    hidden = (jax.nn.gelu(smoothed) * values.astype(f32)).astype(bf16)
    partial = jnp.dot(
        hidden, lax.all_gather(w_down, "sp", axis=1, tiled=True), preferred_element_type=f32
    )
    branch = lax.psum_scatter(partial.astype(bf16), "tp", scatter_dimension=0, tiled=True)
    return normalize(deep_alpha * kept + branch.astype(f32), gain_ffn).astype(bf16)


def hop(value, axis, mask):
    count = lax.axis_size(axis)
    return lax.ppermute(value, axis, [(i, i ^ mask) for i in range(count)])


def doubled(pieces, axis, masks):
    pieces = dict(pieces)
    for mask in masks:
        for have in list(pieces):
            pieces[have ^ mask] = hop(pieces[have], axis, mask)
    return pieces


def norm_kernel(ids_ref, ch_ref, own_ref, gain_ref, *refs, tp):
    wout = refs[:tp]
    far = refs[tp : 2 * tp]
    out_ref = refs[2 * tp]
    far_rows = refs[2 * tp + 1]
    t = ids_ref[1]
    quarter = far[0].shape[0]
    rows = own_ref.shape[0]
    blocks, _, _, block = out_ref.shape
    for m in range(tp):
        start = pl.multiple_of(jnp.bitwise_xor(t, m) * quarter, quarter)
        far_rows[pl.ds(start, quarter), :] = far[m][...]
    gain = gain_ref[...]
    part = min(128, rows)
    for c in range(2):
        for r in range(0, rows, part):
            total = None
            for m in range(tp):
                one = jnp.dot(
                    ch_ref[jnp.bitwise_xor(t, m), c, r : r + part, :], wout[m][...],
                    preferred_element_type=f32,
                )
                total = one if total is None else total + one
            base = own_ref[r : r + part, :] if c == 0 else far_rows[r : r + part, :]
            made = normalize(deep_alpha * base.astype(f32) + total, gain).astype(bf16)
            for b in range(blocks):
                out_ref[b, c, r : r + part, :] = made[:, b * block : (b + 1) * block]


def project(ids_ref, nf_ref, pieces, acc):
    s = ids_ref[0]
    blocks, _, rows, block = nf_ref.shape
    for n, (m, piece) in enumerate(pieces):
        one = jnp.dot(
            nf_ref[jnp.bitwise_xor(s, m)].reshape(2 * rows, block), piece[...],
            preferred_element_type=f32,
        )
        if n == 0:
            acc[...] = one
        else:
            acc[...] = acc[...] + one


def gate_kernel(ids_ref, nf_ref, *refs, masks):
    pieces = list(zip(masks, refs[: len(masks)]))
    gated_ref, head_ref, tail_ref, acc = refs[len(masks) :]
    project(ids_ref, nf_ref, pieces, acc)
    rows = gated_ref.shape[1]
    for c in range(2):
        part = acc[c * rows : (c + 1) * rows, :].astype(bf16)
        gated_ref[c] = part
        head_ref[c : c + 1, :] = acc[c * rows : c * rows + 1, :].astype(bf16)
        tail_ref[c : c + 1, :] = acc[(c + 1) * rows - 1 : (c + 1) * rows, :].astype(bf16)


def value_kernel(ids_ref, nf_ref, gated_ref, before_ref, after_ref, taps_ref, *refs, masks, tp, low_count):
    pieces = list(zip(masks, refs[: len(masks)]))
    hid_ref, acc = refs[len(masks) :]
    project(ids_ref, nf_ref, pieces, acc)
    rows = gated_ref.shape[1]
    units = gated_ref.shape[2]
    t = ids_ref[1]
    s = ids_ref[0]
    hi = s // low_count
    lo = s % low_count
    row = iota((rows, units), 0)
    taps = taps_ref[...]
    quarter = rows // tp
    for c in range(2):
        chunk = jnp.bitwise_xor(hi, c)
        here = gated_ref[c].astype(f32)
        first = before_ref[c : c + 1, :].astype(f32)
        crossed = jnp.where(chunk == 1, before_ref[1 - c : 2 - c, :].astype(f32), 0.0)
        first = jnp.where(lo > 0, first, crossed)
        last = after_ref[c : c + 1, :].astype(f32)
        crossed = jnp.where(chunk == 0, after_ref[1 - c : 2 - c, :].astype(f32), 0.0)
        last = jnp.where(lo < low_count - 1, last, crossed)
        prev = jnp.where(row == 0, first, pltpu.roll(here, 1, 0))
        nxt = jnp.where(row == rows - 1, last, pltpu.roll(here, rows - 1, 0))
        smoothed = taps[0:1] * prev + taps[1:2] * here + taps[2:3] * nxt
        values = acc[c * rows : (c + 1) * rows, :].astype(bf16).astype(f32)
        acc[c * rows : (c + 1) * rows, :] = jax.nn.gelu(smoothed) * values
    bits = [1 << b for b in range(tp.bit_length() - 1)]
    for rel in range(tp):
        place = 0
        for bit in bits:
            place = 2 * place + (1 if rel & bit else 0)
        start = pl.multiple_of(jnp.bitwise_xor(t, rel) * quarter, quarter)
        for c in range(2):
            at = (2 * place + c) * quarter
            hid_ref[at : at + quarter, :] = acc[pl.ds(c * rows + start, quarter), :].astype(bf16)


def down_kernel(ids_ref, hid_ref, *refs, masks, low_count):
    pieces = refs[: len(masks)]
    keep_ref, send_ref = refs[len(masks) :]
    hi = ids_ref[0] // low_count
    mid = keep_ref.shape[2]
    hid = hid_ref[...]
    for n, m in enumerate(masks):
        made = jnp.dot(hid, pieces[n][...], preferred_element_type=f32).astype(bf16)
        column = jnp.bitwise_xor(hi, m // low_count)
        place = (m % low_count) >> 1
        keep_ref[column, place] = made[:mid]
        send_ref[column, place] = made[mid:]


def final_kernel(ids_ref, nf_ref, keep_a, got_a, keep_b, got_b, gain_ref, out_ref, *, low_count):
    blocks, _, _, block = nf_ref.shape
    lo = ids_ref[0] % low_count
    cells = []
    for b in range(blocks):
        mask = jnp.bitwise_xor(lo, b % low_count)
        place = mask >> 1
        col = b // low_count
        first = keep_a[col, place].astype(f32) + got_a[col, place].astype(f32)
        second = keep_b[col, place].astype(f32) + got_b[col, place].astype(f32)
        branch = jnp.where(mask % 2 == 0, first, second)
        cells.append(deep_alpha * nf_ref[b, 0].astype(f32) + branch)
    out_ref[...] = normalize(jnp.concatenate(cells, axis=1), gain_ref[...]).astype(bf16)


def split_mixer(channels, residual, w_out, gain_mix, w_gate, w_value, conv_taps, w_down, gain_ffn):
    count = lax.axis_size("sp")
    tp = lax.axis_size("tp")
    low_count = count // 2
    top = low_count
    s = lax.axis_index("sp")
    t = lax.axis_index("tp")
    hi = s // low_count
    ids = jnp.stack([s, t]).astype(jnp.int32)
    rows, model = residual.shape
    block = model // count
    quarter = rows // tp
    units = w_gate.shape[1] // 2
    low_bits = [1 << b for b in range(low_count.bit_length() - 1)]
    falling = low_bits[::-1]
    tp_masks = [1 << b for b in range(tp.bit_length() - 1)][::-1]

    def halves(weight, dim):
        keep = lax.dynamic_slice_in_dim(weight, hi * units, units, dim)
        send = lax.dynamic_slice_in_dim(weight, (1 - hi) * units, units, dim)
        return keep, send

    def spread_weight(weight, dim, order):
        keep, send = halves(weight, dim)
        return doubled({0: keep, top: hop(send, "sp", top)}, "sp", order)

    gates = spread_weight(w_gate, 1, falling)
    vals = spread_weight(w_value, 1, low_bits)
    downs = spread_weight(w_down, 0, falling)
    outs = doubled({0: w_out}, "tp", tp_masks)
    mine = lax.dynamic_slice_in_dim(residual, t * quarter, quarter, 0)
    fars = doubled({0: hop(mine, "sp", top)}, "tp", tp_masks)
    taps = lax.dynamic_slice_in_dim(conv_taps, hi * units, units, 1)

    pair = jnp.stack([channels, hop(channels, "sp", top)])
    every = lax.all_gather(pair, "tp")

    def norm_body(*refs):
        norm_kernel(*refs, tp=tp)

    nf = pl.pallas_call(
        norm_body,
        out_shape=jax.ShapeDtypeStruct((count, 2, rows, block), bf16),
        in_specs=[scalar_spec()] + [whole_spec()] * (3 + 2 * tp),
        out_specs=whole_spec(),
        scratch_shapes=[pltpu.VMEM((rows, model), bf16)],
        compiler_params=vmem(),
        cost_estimate=cost(4 * rows * model * w_out.shape[0] * tp, 8_000_000),
        name="norm_first",
    )(
        ids, every, residual, gain_mix.reshape(1, model),
        *[outs[m] for m in range(tp)], *[fars[m] for m in range(tp)],
    )

    masks = tuple(range(count))

    def gate_body(*refs):
        gate_kernel(*refs, masks=masks)

    work = 4 * rows * model * units
    gated, heads, tails = pl.pallas_call(
        gate_body,
        out_shape=(
            jax.ShapeDtypeStruct((2, rows, units), bf16),
            jax.ShapeDtypeStruct((2, units), bf16),
            jax.ShapeDtypeStruct((2, units), bf16),
        ),
        in_specs=[scalar_spec()] + [whole_spec()] * (1 + count),
        out_specs=[whole_spec()] * 3,
        scratch_shapes=[pltpu.VMEM((2 * rows, units), f32)],
        compiler_params=vmem(),
        cost_estimate=cost(work, 6_000_000),
        name="gate_rows",
    )(ids, nf, *[gates[m] for m in masks])

    def ring(shift):
        return [
            (h * low_count + l, h * low_count + (l + shift) % low_count)
            for h in range(2)
            for l in range(low_count)
        ]

    before = lax.ppermute(tails, "sp", ring(1))
    after = lax.ppermute(heads, "sp", ring(-1))

    def value_body(*refs):
        value_kernel(*refs, masks=masks, tp=tp, low_count=low_count)

    hidden = pl.pallas_call(
        value_body,
        out_shape=jax.ShapeDtypeStruct((2 * rows, units), bf16),
        in_specs=[scalar_spec()] + [whole_spec()] * (5 + count),
        out_specs=whole_spec(),
        scratch_shapes=[pltpu.VMEM((2 * rows, units), f32)],
        compiler_params=vmem(),
        cost_estimate=cost(work, 6_000_000),
        name="hidden_rows",
    )(ids, nf, gated, before, after, taps, *[vals[m] for m in masks])

    def branch_part(last_bit):
        some = tuple(m for m in masks if m % 2 == last_bit)

        def down_body(*refs):
            down_kernel(*refs, masks=some, low_count=low_count)

        shape = jax.ShapeDtypeStruct((2, low_count // 2, rows, block), bf16)
        keep, send = pl.pallas_call(
            down_body,
            out_shape=(shape, shape),
            in_specs=[scalar_spec()] + [whole_spec()] * (1 + len(some)),
            out_specs=[whole_spec()] * 2,
            compiler_params=vmem(),
            cost_estimate=cost(work // 2, 3_000_000),
            name=f"down_{last_bit}",
        )(ids, hidden, *[downs[m] for m in some])
        for mask in tp_masks[::-1][1:] + [None]:
            got = hop(send, "tp", mask // 2 if mask else tp_masks[0])
            total = (keep.astype(f32) + got.astype(f32)).astype(bf16)
            mid = total.shape[2] // 2
            keep, send = total[:, :, :mid], total[:, :, mid:]
        return keep, hop(send, "sp", top)

    keep_a, got_a = branch_part(0)
    keep_b, got_b = branch_part(1)

    def final_body(*refs):
        final_kernel(*refs, low_count=low_count)

    nf_own = lax.dynamic_slice(nf, (0, 0, t * quarter, 0), (count, 1, quarter, block))
    return pl.pallas_call(
        final_body,
        out_shape=jax.ShapeDtypeStruct((quarter, model), bf16),
        in_specs=[scalar_spec()] + [whole_spec()] * 6,
        out_specs=whole_spec(),
        compiler_params=vmem(),
        cost_estimate=cost(10_000_000, 2_000_000),
        name="result_rows",
    )(ids, nf_own, keep_a, got_a, keep_b, got_b, gain_ffn.reshape(1, model))


def shards(
    residual,
    ssm_input,
    in_map,
    out_map,
    damping,
    log_step,
    frequency,
    pacing,
    feedthrough,
    w_out,
    gain_mix,
    w_gate,
    w_value,
    conv_taps,
    w_down,
    gain_ffn,
):
    channels = ssm_channels(
        ssm_input, in_map, out_map, damping, log_step, frequency, pacing, feedthrough
    )
    count = lax.axis_size("sp")
    tp = lax.axis_size("tp")
    block = residual.shape[1] // count
    powers = count & (count - 1) == 0 and tp & (tp - 1) == 0
    if powers and 4 <= count <= 8 and tp >= 2 and block % LANES == 0:
        mixer = split_mixer
    else:
        mixer = plain_mixer
    return mixer(
        channels, residual, w_out, gain_mix, w_gate, w_value, conv_taps, w_down, gain_ffn
    )


def solution(mesh):
    in_specs = (
        P("sp", None),
        P("sp", "tp"),
        P(None, "tp", None, None),
        P(None, "tp", None, None),
        P("tp", None),
        P("tp"),
        P("tp", None),
        P("sp"),
        P("tp"),
        P("tp", None),
        P(),
        P("sp", "tp"),
        P("sp", "tp"),
        P(None, "tp"),
        P("tp", "sp"),
        P(),
    )
    out_specs = P(("sp", "tp"), None)
    return jax.shard_map(shards, mesh=mesh, in_specs=in_specs, out_specs=out_specs, check_vma=False)
```

```python
import math

import jax
import jax.numpy as jnp
from jax import lax
from jax.experimental import pallas as pl
from jax.experimental.pallas import tpu as pltpu
from jax.sharding import PartitionSpec as P


deep_alpha = 8.0**0.25
norm_eps = 1e-06
SEG = 8
LANES = 128
f32 = jnp.float32
bf16 = jnp.bfloat16
NT = (((1,), (1,)), ((), ()))


ROUTES = {"gate": ["zy", "zy"], "value": ["zy", "zy"], "down": ["yz", "zy"]}


def vmem(limit):
    return pltpu.CompilerParams(vmem_limit_bytes=limit * 1024 * 1024)


def cost(flops, moved):
    return pl.CostEstimate(flops=flops, bytes_accessed=moved, transcendentals=0)


def whole_spec():
    return pl.BlockSpec(memory_space=pltpu.VMEM)


def scalar_spec():
    return pl.BlockSpec(memory_space=pltpu.SMEM)


def iota(shape, dim):
    return lax.broadcasted_iota(jnp.int32, shape, dim)


def cmul(a_re, a_im, b_re, b_im):
    return a_re * b_re - a_im * b_im, a_re * b_im + a_im * b_re


def sin_cos(angle):
    turns = jnp.floor(angle * (2.0 / math.pi) + 0.5)
    rest = ((angle - turns * 1.5703125) - turns * 4.837512969970703125e-4) - (
        turns * 7.54978995489188216e-8
    )
    sq = rest * rest
    sine = ((-1.9515295891e-4 * sq + 8.3321608736e-3) * sq - 1.6666654611e-1) * sq * rest + rest
    cosine = (
        ((2.443315711809948e-5 * sq - 1.388731625493765e-3) * sq + 4.166664568298827e-2) * sq * sq
        - 0.5 * sq
        + 1.0
    )
    quad = turns.astype(jnp.int32)
    swap = (quad & 1) == 1
    sin_out = jnp.where(swap, cosine, sine)
    cos_out = jnp.where(swap, sine, cosine)
    sin_out = jnp.where((quad & 2) == 2, -sin_out, sin_out)
    cos_out = jnp.where(((quad + 1) & 2) == 2, -cos_out, cos_out)
    return sin_out, cos_out


def spread_maps(maps, group_width):
    half = LANES // 2
    rows = maps[0].shape[0]
    lane = iota((rows, LANES), 1)
    low = lane < half
    odd = (iota((rows, LANES), 0) // group_width) % 2 == 1
    match = odd != low
    parts = []
    for one in maps:
        one = one.astype(f32)
        turned = pltpu.roll(one, half, 1)
        parts.append(jnp.where(match, jnp.where(low, one, turned), 0.0))
        parts.append(jnp.where(match, jnp.where(low, turned, one), 0.0))
    return jnp.concatenate(parts, axis=1).astype(bf16)


def state_kernel(
    u_ref, in_ref, out_ref, damp_ref, freq_ref, logs_ref, pace_ref,
    ro_ref, dec_ref, seg_ref, sum_ref,
    tab, wide_in, wide_out, u_perm, drv, st, pc,
):
    length = u_ref.shape[0]
    groups = damp_ref.shape[0]
    half = damp_ref.shape[1]
    width = u_ref.shape[1] // groups
    steps = length // SEG
    tiles = groups // 2
    step = jnp.exp(logs_ref[...])
    diag = iota((groups, groups), 0) == iota((groups, groups), 1)
    step_col = jnp.sum(jnp.where(diag, jnp.broadcast_to(step, (groups, groups)), 0.0), axis=1, keepdims=True)
    rate_re = -damp_ref[...]
    rate_im = freq_ref[...]
    modulus = rate_re * rate_re + rate_im * rate_im
    rows = (rate_re * step_col, rate_im * step_col, rate_re / modulus, -rate_im / modulus)
    low = iota((1, LANES), 1) < half
    for which, table in enumerate(rows):
        twice = jnp.concatenate([table, table], axis=1)
        for k in range(tiles):
            tab[k, which : which + 1, :] = jnp.where(low, twice[2 * k : 2 * k + 1], twice[2 * k + 1 : 2 * k + 2])
    wide_in[...] = spread_maps((in_ref[0], in_ref[1]), width)
    wide_out[...] = spread_maps((out_ref[0], out_ref[1]), width)
    r_id = iota((length, length), 0)
    t_id = iota((length, length), 1)
    pick = t_id == (r_id % SEG) * steps + r_id // SEG
    u_perm[...] = jnp.dot(
        jnp.where(pick, 1.0, 0.0).astype(bf16), u_ref[...], preferred_element_type=f32
    ).astype(bf16)
    pace_col = jnp.sum(
        jnp.where(pick, jnp.broadcast_to(pace_ref[...], (length, length)), 0.0), axis=1, keepdims=True
    )
    pc[...] = jnp.broadcast_to(pace_col, (length, LANES))
    ro_ref[...] = jnp.zeros_like(ro_ref)
    col_tile = iota((length, u_ref.shape[1]), 1) // (2 * width)

    def per_tile(k, carry):
        pace = pc[...]
        magnitude = jnp.exp(tab[k, 0:1, :] * pace)
        sine, cosine = sin_cos(tab[k, 1:2, :] * pace)
        dec_re = magnitude * cosine
        dec_im = magnitude * sine
        dec_ref[0, k] = dec_re
        dec_ref[1, k] = dec_im
        inv_re = tab[k, 2:3, :]
        inv_im = tab[k, 3:4, :]
        fac_re, fac_im = cmul(dec_re - 1.0, dec_im, inv_re, inv_im)
        mine = jnp.where(col_tile == k, u_perm[...].astype(f32), 0.0).astype(bf16)
        inflow = jnp.dot(mine, wide_in[...], preferred_element_type=f32)
        for d in range(2):
            x_re = inflow[:, 2 * d * LANES : (2 * d + 1) * LANES]
            x_im = inflow[:, (2 * d + 1) * LANES : (2 * d + 2) * LANES]
            a, b = cmul(fac_re, fac_im, x_re, x_im)
            drv[2 * d] = a
            drv[2 * d + 1] = b
        h_re = jnp.zeros((SEG, LANES), f32)
        h_im = h_re
        g_re = h_re
        g_im = h_re
        p_re = jnp.ones((SEG, LANES), f32)
        p_im = h_re
        for i in range(steps):
            lo = i * SEG
            d_re = dec_ref[0, k, lo : lo + SEG, :]
            d_im = dec_ref[1, k, lo : lo + SEG, :]
            h_re, h_im = cmul(d_re, d_im, h_re, h_im)
            h_re = h_re + drv[0, lo : lo + SEG, :]
            h_im = h_im + drv[1, lo : lo + SEG, :]
            st[lo : lo + SEG, 0:LANES] = h_re
            st[lo : lo + SEG, LANES : 2 * LANES] = h_im
            p_re, p_im = cmul(d_re, d_im, p_re, p_im)
            hi = (steps - 1 - i) * SEG
            d_re = dec_ref[0, k, hi : hi + SEG, :]
            d_im = dec_ref[1, k, hi : hi + SEG, :]
            g_re, g_im = cmul(d_re, d_im, g_re, g_im)
            g_re = g_re + drv[2, hi : hi + SEG, :]
            g_im = g_im + drv[3, hi : hi + SEG, :]
            st[hi : hi + SEG, 2 * LANES : 3 * LANES] = g_re
            st[hi : hi + SEG, 3 * LANES : 4 * LANES] = g_im
        ends = (p_re, p_im, h_re, h_im, g_re, g_im)
        for q in range(6):
            seg_ref[k, q] = ends[q]
        t_re = jnp.ones((1, LANES), f32)
        t_im = jnp.zeros((1, LANES), f32)
        f_re = t_im
        f_im = t_im
        b_re = t_im
        b_im = t_im
        for j in range(SEG):
            one = [e[j : j + 1] for e in ends]
            t_re, t_im = cmul(one[0], one[1], t_re, t_im)
            f_re, f_im = cmul(one[0], one[1], f_re, f_im)
            f_re = f_re + one[2]
            f_im = f_im + one[3]
            o = SEG - 1 - j
            one = [e[o : o + 1] for e in ends]
            b_re, b_im = cmul(one[0], one[1], b_re, b_im)
            b_re = b_re + one[4]
            b_im = b_im + one[5]
        for q, row in enumerate((t_re, t_im, f_re, f_im, b_re, b_im)):
            sum_ref[q, pl.ds(k, 1), :] = row
        states = st[...]
        upper = states.astype(bf16)
        lower = (states - upper.astype(f32)).astype(bf16)
        got = lax.dot_general(upper, wide_out[...], NT, preferred_element_type=f32)
        got = got + lax.dot_general(lower, wide_out[...], NT, preferred_element_type=f32)
        ro_ref[...] = jnp.where(col_tile == k, got, ro_ref[...])
        return carry

    lax.fori_loop(0, tiles, per_tile, 0)


def carry_kernel(
    ids_ref, dec_ref, seg_ref, ro_ref, u_ref, feed_ref, out_ref, *refs, count, relative,
):
    ch_ref, wide_out, acc, st, car, pad, gat_ref = refs[-7:]
    filled = 0
    for part in refs[:-7]:
        gat_ref[filled : filled + part.shape[0]] = part[...]
        filled += part.shape[0]
    length = u_ref.shape[0]
    channels = u_ref.shape[1]
    tiles = dec_ref.shape[1]
    width = channels // (2 * tiles)
    steps = length // SEG
    mine = ids_ref[0]
    wide_out[...] = spread_maps((out_ref[0], out_ref[1]), width)
    zero = jnp.zeros((tiles, LANES), f32)

    def fold(n, state):
        f_re, f_im, b_re, b_im = state
        here = n
        at = jnp.bitwise_xor(here, mine) if relative else here
        a, b = cmul(gat_ref[at, 0], gat_ref[at, 1], f_re, f_im)
        ok = here < mine
        f_re = jnp.where(ok, a + gat_ref[at, 2], f_re)
        f_im = jnp.where(ok, b + gat_ref[at, 3], f_im)
        here = count - 1 - n
        at = jnp.bitwise_xor(here, mine) if relative else here
        a, b = cmul(gat_ref[at, 0], gat_ref[at, 1], b_re, b_im)
        ok = here > mine
        b_re = jnp.where(ok, a + gat_ref[at, 4], b_re)
        b_im = jnp.where(ok, b + gat_ref[at, 5], b_im)
        return f_re, f_im, b_re, b_im

    for q, value in enumerate(lax.fori_loop(0, count, fold, (zero, zero, zero, zero))):
        car[q] = value
    acc[...] = ro_ref[...]
    col_tile = iota((length, channels), 1) // (2 * width)

    def per_tile(k, carry):
        f_re = car[0, pl.ds(k, 1), :]
        f_im = car[1, pl.ds(k, 1), :]
        b_re = car[2, pl.ds(k, 1), :]
        b_im = car[3, pl.ds(k, 1), :]
        for j in range(SEG):
            pad[0, j : j + 1, :] = f_re
            pad[1, j : j + 1, :] = f_im
            a, b = cmul(seg_ref[k, 0, j : j + 1, :], seg_ref[k, 1, j : j + 1, :], f_re, f_im)
            f_re = a + seg_ref[k, 2, j : j + 1, :]
            f_im = b + seg_ref[k, 3, j : j + 1, :]
            o = SEG - 1 - j
            pad[2, o : o + 1, :] = b_re
            pad[3, o : o + 1, :] = b_im
            a, b = cmul(seg_ref[k, 0, o : o + 1, :], seg_ref[k, 1, o : o + 1, :], b_re, b_im)
            b_re = a + seg_ref[k, 4, o : o + 1, :]
            b_im = b + seg_ref[k, 5, o : o + 1, :]
        h_re = pad[0]
        h_im = pad[1]
        g_re = pad[2]
        g_im = pad[3]
        for i in range(steps):
            lo = i * SEG
            h_re, h_im = cmul(dec_ref[0, k, lo : lo + SEG, :], dec_ref[1, k, lo : lo + SEG, :], h_re, h_im)
            st[lo : lo + SEG, 0:LANES] = h_re
            st[lo : lo + SEG, LANES : 2 * LANES] = h_im
            hi = (steps - 1 - i) * SEG
            g_re, g_im = cmul(dec_ref[0, k, hi : hi + SEG, :], dec_ref[1, k, hi : hi + SEG, :], g_re, g_im)
            st[hi : hi + SEG, 2 * LANES : 3 * LANES] = g_re
            st[hi : hi + SEG, 3 * LANES : 4 * LANES] = g_im
        states = st[...]
        upper = states.astype(bf16)
        lower = (states - upper.astype(f32)).astype(bf16)
        got = lax.dot_general(upper, wide_out[...], NT, preferred_element_type=f32)
        got = got + lax.dot_general(lower, wide_out[...], NT, preferred_element_type=f32)
        acc[...] = acc[...] + jnp.where(col_tile == k, got, 0.0)
        return carry

    lax.fori_loop(0, tiles, per_tile, 0)
    r_id = iota((length, length), 0)
    t_id = iota((length, length), 1)
    pick = jnp.where(t_id == (r_id % SEG) * steps + r_id // SEG, 1.0, 0.0).astype(bf16)
    u_perm = jnp.dot(pick, u_ref[...], preferred_element_type=f32)
    made = jax.nn.gelu(acc[...] + feed_ref[...] * u_perm).astype(bf16)
    unpick = jnp.where(r_id == (t_id % SEG) * steps + t_id // SEG, 1.0, 0.0).astype(bf16)
    ch_ref[...] = jnp.dot(unpick, made, preferred_element_type=f32).astype(bf16)


def ssm_channels(ssm_input, in_map, out_map, damping, log_step, frequency, pacing, feedthrough):
    length, channels = ssm_input.shape
    groups, half = damping.shape
    tiles = groups // 2
    count = lax.axis_size("sp")
    in_rows = in_map.reshape(2, channels, 2 * half)
    out_rows = out_map.reshape(2, channels, 2 * half)
    ro, dec, seg, summary = pl.pallas_call(
        state_kernel,
        out_shape=(
            jax.ShapeDtypeStruct((length, channels), f32),
            jax.ShapeDtypeStruct((2, tiles, length, LANES), f32),
            jax.ShapeDtypeStruct((tiles, 6, SEG, LANES), f32),
            jax.ShapeDtypeStruct((6, tiles, LANES), f32),
        ),
        in_specs=[whole_spec()] * 7,
        out_specs=[whole_spec()] * 4,
        scratch_shapes=[
            pltpu.VMEM((tiles, 8, LANES), f32),
            pltpu.VMEM((channels, 4 * LANES), bf16),
            pltpu.VMEM((channels, 4 * LANES), bf16),
            pltpu.VMEM((length, channels), bf16),
            pltpu.VMEM((4, length, LANES), f32),
            pltpu.VMEM((length, 4 * LANES), f32),
            pltpu.VMEM((length, LANES), f32),
        ],
        compiler_params=vmem(14),
        cost_estimate=cost(2_000_000_000, 4_000_000),
        name="state_pass",
    )(
        ssm_input, in_rows, out_rows, damping, frequency,
        log_step.reshape(1, groups), pacing.reshape(1, length),
    )
    relative = count & (count - 1) == 0 and count <= 16
    if relative:
        gathered = [summary[None]]
        step = 1
        while step < count:
            whole = gathered[0] if len(gathered) == 1 else jnp.concatenate(gathered, axis=0)
            gathered = [whole, hop(whole, "sp", step)]
            step *= 2
    else:
        gathered = [lax.all_gather(summary, "sp")]
    ids = jnp.stack([lax.axis_index("sp")]).astype(jnp.int32)

    def body(*refs):
        carry_kernel(*refs, count=count, relative=relative)

    return pl.pallas_call(
        body,
        out_shape=jax.ShapeDtypeStruct((length, channels), bf16),
        in_specs=[scalar_spec()] + [whole_spec()] * (6 + len(gathered)),
        out_specs=whole_spec(),
        scratch_shapes=[
            pltpu.VMEM((channels, 4 * LANES), bf16),
            pltpu.VMEM((length, channels), f32),
            pltpu.VMEM((length, 4 * LANES), f32),
            pltpu.VMEM((4, tiles, LANES), f32),
            pltpu.VMEM((4, SEG, LANES), f32),
            pltpu.VMEM((count, 6, tiles, LANES), f32),
        ],
        compiler_params=vmem(12),
        cost_estimate=cost(2_000_000_000, 4_000_000),
        name="carry_pass",
    )(ids, dec, seg, ro, ssm_input, feedthrough.reshape(1, channels), out_rows, *gathered)


def normalize(pre_norm, gain_row):
    mean_row = jnp.mean(pre_norm, axis=-1, keepdims=True)
    centred = pre_norm - mean_row
    spread = jnp.mean(centred * centred, axis=-1, keepdims=True)
    return centred * lax.rsqrt(spread + norm_eps) * gain_row


def plain_mixer(channels, residual, w_out, gain_mix, w_gate, w_value, conv_taps, w_down, gain_ffn):
    own_rows = residual.shape[0] // lax.axis_size("tp")
    mixed = lax.psum(
        jnp.dot(channels, w_out, preferred_element_type=f32).astype(bf16), "tp"
    ).astype(f32)
    rows = normalize(deep_alpha * residual.astype(f32) + mixed, gain_mix).astype(bf16)
    kept = lax.dynamic_slice_in_dim(rows, lax.axis_index("tp") * own_rows, own_rows, 0).astype(f32)
    gated = jnp.dot(
        rows, lax.all_gather(w_gate, "sp", axis=0, tiled=True), preferred_element_type=f32
    ).astype(bf16)
    values = jnp.dot(
        rows, lax.all_gather(w_value, "sp", axis=0, tiled=True), preferred_element_type=f32
    ).astype(bf16)
    count = lax.axis_size("sp")
    before = lax.ppermute(gated[-1:], "sp", [(i, i + 1) for i in range(count - 1)])
    after = lax.ppermute(gated[:1], "sp", [(i + 1, i) for i in range(count - 1)])
    padded = jnp.concatenate([before, gated, after], axis=0).astype(f32)
    smoothed = conv_taps[0] * padded[:-2] + conv_taps[1] * padded[1:-1] + conv_taps[2] * padded[2:]
    hidden = (jax.nn.gelu(smoothed) * values.astype(f32)).astype(bf16)
    partial = jnp.dot(
        hidden, lax.all_gather(w_down, "sp", axis=1, tiled=True), preferred_element_type=f32
    )
    branch = lax.psum_scatter(partial.astype(bf16), "tp", scatter_dimension=0, tiled=True)
    return normalize(deep_alpha * kept + branch.astype(f32), gain_ffn).astype(bf16)


def hop(value, axis, mask):
    count = lax.axis_size(axis)
    return lax.ppermute(value, axis, [(i, i ^ mask) for i in range(count)])


def doubled(pieces, axis, masks):
    pieces = dict(pieces)
    for mask in masks:
        for have in list(pieces):
            pieces[have ^ mask] = hop(pieces[have], axis, mask)
    return pieces


def joined(value, axis, masks):
    have = value[None]
    got = None
    for mask in masks:
        if got is not None:
            have = jnp.concatenate([have, got], axis=0)
        got = hop(have, axis, mask)
    return have, got


def joined_place(member, masks):
    index = 0
    for k, mask in enumerate(masks[:-1]):
        index += (1 if member & mask else 0) << k
    return (1 if member & masks[-1] else 0), index


def norm_kernel(ids_ref, ch_0, ch_1, far_0, far_1, own_ref, gain_ref, *refs, tp, tp_masks):
    wout = refs[:tp]
    out_ref, kept_ref, far_rows, pre = refs[tp:]
    t = ids_ref[1]
    quarter = far_0.shape[1]
    rows = own_ref.shape[0]
    blocks, _, _, block = out_ref.shape
    depth = ch_0.shape[-1]
    places = [joined_place(m, tp_masks) for m in range(tp)]
    for m, (side, at) in enumerate(places):
        start = pl.multiple_of(jnp.bitwise_xor(t, m) * quarter, quarter)
        far_rows[pl.ds(start, quarter), :] = (far_0, far_1)[side][at]
    for b in range(blocks):
        total = None
        for m, (side, at) in enumerate(places):
            one = jnp.dot(
                (ch_0, ch_1)[side][at].reshape(2 * rows, depth),
                wout[m][:, b * block : (b + 1) * block],
                preferred_element_type=f32,
            )
            total = one if total is None else total + one
        pre[:, b * block : (b + 1) * block] = total
    gain = gain_ref[...]
    part = min(64, rows)
    for c in range(2):
        base = own_ref if c == 0 else far_rows
        for r in range(0, rows, part):
            lo = c * rows + r
            made = normalize(
                deep_alpha * base[r : r + part, :].astype(f32) + pre[lo : lo + part, :], gain
            )
            if c == 0:
                pre[lo : lo + part, :] = made
            made = made.astype(bf16)
            for b in range(blocks):
                out_ref[b, c, r : r + part, :] = made[:, b * block : (b + 1) * block]
    kept_ref[...] = pre[pl.ds(pl.multiple_of(t * quarter, quarter), quarter), :].astype(bf16)


def project(ids_ref, nf_ref, pieces):
    s = ids_ref[0]
    _, _, rows, block = nf_ref.shape
    total = None
    for m, piece in pieces:
        one = jnp.dot(
            nf_ref[jnp.bitwise_xor(s, m)].reshape(2 * rows, block), piece[...],
            preferred_element_type=f32,
        )
        total = one if total is None else total + one
    return total.astype(bf16)


def gate_kernel(ids_ref, nf_ref, *refs, masks):
    pieces = list(zip(masks, refs[: len(masks)]))
    gated_ref, head_ref, tail_ref = refs[len(masks) :]
    total = project(ids_ref, nf_ref, pieces)
    rows = gated_ref.shape[1]
    for c in range(2):
        gated_ref[c] = total[c * rows : (c + 1) * rows]
        head_ref[c : c + 1, :] = total[c * rows : c * rows + 1]
        tail_ref[c : c + 1, :] = total[(c + 1) * rows - 1 : (c + 1) * rows]


def value_kernel(ids_ref, nf_ref, *refs, masks):
    pieces = list(zip(masks, refs[: len(masks)]))
    values_ref = refs[len(masks)]
    values_ref[...] = project(ids_ref, nf_ref, pieces).reshape(values_ref.shape)


def make_hidden(ids_ref, gated_ref, values_ref, before_ref, after_ref, taps_ref, hid_ref, made, tp, low_count):
    rows = gated_ref.shape[1]
    units = gated_ref.shape[2]
    t = ids_ref[1]
    s = ids_ref[0]
    hi = s // low_count
    lo = s % low_count
    row = iota((rows, units), 0)
    taps = taps_ref[...]
    quarter = rows // tp
    for c in range(2):
        chunk = jnp.bitwise_xor(hi, c)
        here = gated_ref[c].astype(f32)
        first = before_ref[c : c + 1, :].astype(f32)
        crossed = jnp.where(chunk == 1, before_ref[1 - c : 2 - c, :].astype(f32), 0.0)
        first = jnp.where(lo > 0, first, crossed)
        last = after_ref[c : c + 1, :].astype(f32)
        crossed = jnp.where(chunk == 0, after_ref[1 - c : 2 - c, :].astype(f32), 0.0)
        last = jnp.where(lo < low_count - 1, last, crossed)
        prev = jnp.where(row == 0, first, pltpu.roll(here, 1, 0))
        nxt = jnp.where(row == rows - 1, last, pltpu.roll(here, rows - 1, 0))
        smoothed = taps[0:1] * prev + taps[1:2] * here + taps[2:3] * nxt
        made[c * rows : (c + 1) * rows, :] = (
            jax.nn.gelu(smoothed) * values_ref[c].astype(f32)
        ).astype(bf16)
    bits = [1 << b for b in range(tp.bit_length() - 1)]
    for rel in range(tp):
        place = 0
        for bit in bits:
            place = 2 * place + (1 if rel & bit else 0)
        start = pl.multiple_of(jnp.bitwise_xor(t, rel) * quarter, quarter)
        for c in range(2):
            at = (2 * place + c) * quarter
            hid_ref[at : at + quarter, :] = made[pl.ds(c * rows + start, quarter), :]


def down_parts(ids_ref, hid, pieces, keep_ref, send_ref, masks, low_count):
    hi = ids_ref[0] // low_count
    mid = keep_ref.shape[2]
    lows = sorted({m % low_count for m in masks})
    for n, m in enumerate(masks):
        made = jnp.dot(hid, pieces[n][...], preferred_element_type=f32).astype(bf16)
        column = jnp.bitwise_xor(hi, m // low_count)
        place = lows.index(m % low_count)
        keep_ref[column, place] = made[:mid]
        send_ref[column, place] = made[mid:]


def first_down_kernel(
    ids_ref, gated_ref, values_ref, before_ref, after_ref, taps_ref, *refs, masks, tp, low_count
):
    pieces = refs[: len(masks)]
    hid_ref, keep_ref, send_ref, made = refs[len(masks) :]
    make_hidden(
        ids_ref, gated_ref, values_ref, before_ref, after_ref, taps_ref, hid_ref, made, tp, low_count
    )
    down_parts(ids_ref, hid_ref[...], pieces, keep_ref, send_ref, masks, low_count)


def down_kernel(ids_ref, hid_ref, *refs, masks, low_count):
    pieces = refs[: len(masks)]
    keep_ref, send_ref = refs[len(masks) :]
    down_parts(ids_ref, hid_ref[...], pieces, keep_ref, send_ref, masks, low_count)


def final_kernel(ids_ref, nf_ref, keep_a, got_a, keep_b, got_b, gain_ref, out_ref, *, low_count):
    block = keep_a.shape[-1]
    blocks = nf_ref.shape[1] // block
    lo = ids_ref[0] % low_count
    cells = []
    for b in range(blocks):
        mask = jnp.bitwise_xor(lo, b % low_count)
        half = low_count // 2
        place = mask % half
        col = b // low_count
        first = keep_a[col, place].astype(f32) + got_a[col, place].astype(f32)
        second = keep_b[col, place].astype(f32) + got_b[col, place].astype(f32)
        branch = jnp.where(mask < half, first, second)
        cells.append(deep_alpha * nf_ref[:, b * block : (b + 1) * block].astype(f32) + branch)
    out_ref[...] = normalize(jnp.concatenate(cells, axis=1), gain_ref[...]).astype(bf16)


def split_mixer(channels, residual, w_out, gain_mix, w_gate, w_value, conv_taps, w_down, gain_ffn):
    count = lax.axis_size("sp")
    tp = lax.axis_size("tp")
    low_count = count // 2
    top = low_count
    s = lax.axis_index("sp")
    t = lax.axis_index("tp")
    hi = s // low_count
    ids = jnp.stack([s, t]).astype(jnp.int32)
    rows, model = residual.shape
    block = model // count
    quarter = rows // tp
    units = w_gate.shape[1] // 2
    low_bits = [1 << b for b in range(low_count.bit_length() - 1)]
    falling = low_bits[::-1]
    tp_masks = [1 << b for b in range(tp.bit_length() - 1)][::-1]

    def halves(weight, dim):
        keep = lax.dynamic_slice_in_dim(weight, hi * units, units, dim)
        send = lax.dynamic_slice_in_dim(weight, (1 - hi) * units, units, dim)
        return keep, send

    def spread_weight(weight, dim, name):
        near_order, far_order = [falling if r == "zy" else low_bits for r in ROUTES[name]]
        keep, send = halves(weight, dim)
        came = hop(send, "sp", top)
        return doubled({0: keep}, "sp", near_order) | doubled({top: came}, "sp", far_order)

    gates = spread_weight(w_gate, 1, "gate")
    vals = spread_weight(w_value, 1, "value")
    downs = spread_weight(w_down, 0, "down")
    outs = doubled({0: w_out}, "tp", tp_masks)
    mine = lax.dynamic_slice_in_dim(residual, t * quarter, quarter, 0)
    mine = hop(mine, "sp", top)
    fars = joined(mine, "tp", tp_masks)
    taps = lax.dynamic_slice_in_dim(conv_taps, hi * units, units, 1)

    pair = jnp.stack([channels, hop(channels, "sp", top)])
    every = joined(pair, "tp", tp_masks)

    def norm_body(*refs):
        norm_kernel(*refs, tp=tp, tp_masks=tp_masks)

    nf, kept = pl.pallas_call(
        norm_body,
        out_shape=(
            jax.ShapeDtypeStruct((count, 2, rows, block), bf16),
            jax.ShapeDtypeStruct((quarter, model), bf16),
        ),
        in_specs=[scalar_spec()] + [whole_spec()] * (6 + tp),
        out_specs=[whole_spec()] * 2,
        scratch_shapes=[pltpu.VMEM((rows, model), bf16), pltpu.VMEM((2 * rows, model), f32)],
        compiler_params=vmem(22),
        cost_estimate=cost(4 * rows * model * w_out.shape[0] * tp, 8_000_000),
        name="norm_first",
    )(
        ids, *every, *fars, residual, gain_mix.reshape(1, model), *[outs[m] for m in range(tp)],
    )

    masks = tuple(range(count))

    def gate_body(*refs):
        gate_kernel(*refs, masks=masks)

    work = 4 * rows * model * units
    gated, heads, tails = pl.pallas_call(
        gate_body,
        out_shape=(
            jax.ShapeDtypeStruct((2, rows, units), bf16),
            jax.ShapeDtypeStruct((2, units), bf16),
            jax.ShapeDtypeStruct((2, units), bf16),
        ),
        in_specs=[scalar_spec()] + [whole_spec()] * (1 + count),
        out_specs=[whole_spec()] * 3,
        compiler_params=vmem(12),
        cost_estimate=cost(work, 6_000_000),
        name="gate_rows",
    )(ids, nf, *[gates[m] for m in masks])

    def ring(shift):
        return [
            (h * low_count + l, h * low_count + (l + shift) % low_count)
            for h in range(2)
            for l in range(low_count)
        ]

    before = lax.ppermute(tails, "sp", ring(1))
    after = lax.ppermute(heads, "sp", ring(-1))

    def value_body(*refs):
        value_kernel(*refs, masks=masks)

    values = pl.pallas_call(
        value_body,
        out_shape=jax.ShapeDtypeStruct((2, rows, units), bf16),
        in_specs=[scalar_spec()] + [whole_spec()] * (1 + count),
        out_specs=whole_spec(),
        compiler_params=vmem(12),
        cost_estimate=cost(work, 6_000_000),
        name="value_rows",
    )(ids, nf, *[vals[m] for m in masks])

    def summed(keep, send):
        for mask in tp_masks[::-1]:
            got = hop(send, "tp", mask)
            total = (keep.astype(f32) + got.astype(f32)).astype(bf16)
            mid = total.shape[2] // 2
            keep, send = total[:, :, :mid], total[:, :, mid:]
        return keep, hop(send, "sp", top)

    early = tuple(m for m in masks if m % low_count < low_count // 2)
    late = tuple(m for m in masks if m % low_count >= low_count // 2)

    def first_body(*refs):
        first_down_kernel(*refs, masks=early, tp=tp, low_count=low_count)

    shape = jax.ShapeDtypeStruct((2, len(early) // 2, rows, block), bf16)
    hidden, keep, send = pl.pallas_call(
        first_body,
        out_shape=(jax.ShapeDtypeStruct((2 * rows, units), bf16), shape, shape),
        in_specs=[scalar_spec()] + [whole_spec()] * (5 + len(early)),
        out_specs=[whole_spec()] * 3,
        scratch_shapes=[pltpu.VMEM((2 * rows, units), bf16)],
        compiler_params=vmem(14),
        cost_estimate=cost(work // 2, 4_000_000),
        name="down_0",
    )(ids, gated, values, before, after, taps, *[downs[m] for m in early])
    keep_a, got_a = summed(keep, send)

    def late_body(*refs):
        down_kernel(*refs, masks=late, low_count=low_count)

    shape = jax.ShapeDtypeStruct((2, len(late) // 2, rows, block), bf16)
    keep, send = pl.pallas_call(
        late_body,
        out_shape=(shape, shape),
        in_specs=[scalar_spec()] + [whole_spec()] * (1 + len(late)),
        out_specs=[whole_spec()] * 2,
        compiler_params=vmem(10),
        cost_estimate=cost(work // 2, 3_000_000),
        name="down_1",
    )(ids, hidden, *[downs[m] for m in late])
    keep_b, got_b = summed(keep, send)

    def final_body(*refs):
        final_kernel(*refs, low_count=low_count)

    return pl.pallas_call(
        final_body,
        out_shape=jax.ShapeDtypeStruct((quarter, model), bf16),
        in_specs=[scalar_spec()] + [whole_spec()] * 6,
        out_specs=whole_spec(),
        compiler_params=vmem(6),
        cost_estimate=cost(10_000_000, 2_000_000),
        name="result_rows",
    )(ids, kept, keep_a, got_a, keep_b, got_b, gain_ffn.reshape(1, model))


def splits(count, tp):
    return count == 8 and tp == 4


def layer(
    residual, ssm_input, in_map, out_map, damping, log_step, frequency, pacing, feedthrough,
    w_out, gain_mix, w_gate, w_value, conv_taps, w_down, gain_ffn,
):
    channels = ssm_channels(
        ssm_input, in_map, out_map, damping, log_step, frequency, pacing, feedthrough
    )
    count = lax.axis_size("sp")
    tp = lax.axis_size("tp")
    block = residual.shape[1] // count
    if splits(count, tp) and block % LANES == 0:
        mixer = split_mixer
    else:
        mixer = plain_mixer
    return mixer(
        channels, residual, w_out, gain_mix, w_gate, w_value, conv_taps, w_down, gain_ffn
    )


def solution(mesh):
    in_specs = (
        P("sp", None),
        P("sp", "tp"),
        P(None, "tp", None, None),
        P(None, "tp", None, None),
        P("tp", None),
        P("tp"),
        P("tp", None),
        P("sp"),
        P("tp"),
        P("tp", None),
        P(),
        P("sp", "tp"),
        P("sp", "tp"),
        P(None, "tp"),
        P("tp", "sp"),
        P(),
    )
    out_specs = P(("sp", "tp"), None)
    return jax.shard_map(layer, mesh=mesh, in_specs=in_specs, out_specs=out_specs, check_vma=False)
```
